128 devices in a mesh: ep: 32 (over z, y, core), tp: 4 (over x).
Axes of the slice: x: 4, y: 4, z: 4, core: 2. Of those that a mesh axis runs over, the one named last changes fastest.
Arguments:
- q_latent: bfloat16 [16384, 1024], P(('ep', 'tp')), may hold values from -6 to 6
- kv_latent: bfloat16 [16384, 512], P(('ep', 'tp')), may hold values from -8 to 8
- rope_key: bfloat16 [16384, 64], P(('ep', 'tp')), may hold values from -2500 to 2500
- gain_query: float32 [1024], replicated, may hold values from 0.1 to 1.9
- gain_latent: float32 [512], replicated, may hold values from 0.1 to 1.9
- w_query: bfloat16 [1024, 3072], P(None, 'tp'), may hold values from -0.1875 to 0.1875
- w_key: bfloat16 [512, 2048], P(None, 'tp'), may hold values from -0.625 to 0.625
- w_value: bfloat16 [512, 2048], P(None, 'tp'), may hold values from -0.25 to 0.25
- w_out: bfloat16 [2048, 4096], P('tp'), may hold values from -0.25 to 0.25
- tokens_b: bfloat16 [16384, 4096], P(('ep', 'tp')), may hold values from -6 to 6
- gain_norm: float32 [4096], replicated, may hold values from 0.1 to 1.9
- routes: int32 [16384, 2], P(('ep', 'tp')), may hold values from 0 to 31, all different within a row; in each aligned block of 128 rows (0 to 127, 128 to 255, ...) at most 10 rows name the same one
- route_weights: float32 [16384, 2], P(('ep', 'tp')), may hold values from 0.2 to 1
- shared_gate: bfloat16 [4096, 1024], P(None, 'tp'), may hold values from -0.09375 to 0.09375
- shared_up: bfloat16 [4096, 1024], P(None, 'tp'), may hold values from -0.09375 to 0.09375
- shared_down: bfloat16 [1024, 4096], P('tp'), may hold values from -0.1875 to 0.1875
- expert_gate: bfloat16 [32, 4096, 1024], P('ep', None, 'tp'), may hold values from -0.09375 to 0.09375
- expert_up: bfloat16 [32, 4096, 1024], P('ep', None, 'tp'), may hold values from -0.09375 to 0.09375
- expert_down: bfloat16 [32, 1024, 4096], P('ep', 'tp'), may hold values from -0.1875 to 0.1875
Outputs:
- mixer_out: bfloat16 [16384, 4096], P(('ep', 'tp'))
- expert_mix: bfloat16 [16384, 4096], P(('ep', 'tp'))
The draws below stay inside these ranges and needn't reach their ends.
Inputs may be any that keep to these rules, and one draw needn't show every extreme that they name: `routes`: in each aligned block of 128 rows no expert is named by more than 10 rows.
All inputs are finite; a program needn't handle non-finite values.
Results may differ from the reference program's by a relative error of at most 0.018.
The reference program's roundings to bfloat16 on the way count: a program that leaves them out, or rounds other values in their place, can miss the bound.
Values may be sent and summed in bfloat16 or wider, within the bound.
No kernel may reach another device: no remote copies, remote signals or barrier semaphores. Data moves between devices by JAX's collectives and lax.ppermute only.
A program may use at most 192 MiB of HBM per device.

```python
import math
import jax
import jax.numpy as jnp
import numpy as np
from jax import lax

D = 4096
HEADS = 16
NOPE = 128
ROPE = 64
VDIM = 128
QLAT = 1024
KVLAT = 512
FF = 1024
TOP_K = 2
TOK_DEV = 128
EXPERTS = 32
CAPQ = 10
TOKENS = 16384
LENGTH = 16384
N_TP = 4


def draw_rope_key(key, part):
    normal_rows = jnp.clip(jax.random.normal(key, (TOKENS, ROPE), jnp.float32), -6.0, 6.0)
    return normal_rows.astype(jnp.bfloat16)


def draw_kv_latent(key, part):
    noise_key, common_key = jax.random.split(jax.random.fold_in(key, 5))
    block_total = TOKENS // TOK_DEV
    common = jnp.clip(jax.random.normal(common_key, (block_total, KVLAT), jnp.float32), -3.0, 3.0)
    noise = 0.8 * jnp.clip(jax.random.normal(noise_key, (TOKENS, KVLAT), jnp.float32), -6.0, 6.0)
    rows = noise + jnp.repeat(common, TOK_DEV, axis=0)
    return rows.astype(jnp.bfloat16)


def level_of(stream_key, shape, cuts, low, high):
    def one(axis_at, shards_of):
        steps = jax.random.uniform(jax.random.fold_in(jax.random.fold_in(stream_key, 6), axis_at), (shards_of,), jnp.float32, low / len(cuts), high / len(cuts))
        return jnp.repeat(jnp.exp(steps), shape[axis_at] // shards_of).reshape((-1,) + (1,) * (len(shape) - axis_at - 1))

    loudness = one(*cuts[0])
    for cut in cuts[1:]:
        loudness = loudness * one(*cut)
    return loudness


def shared_out(key, own, number, rows, number_of, top, most, skew):
    ranking = jax.random.permutation(key, number_of)
    packed, usual = shares(number_of, rows * top, most, skew, True), shares(number_of, rows * top, most, skew, False)
    places = jnp.arange(number_of)

    def named(tallies, offset_by):
        used = int((tallies > 0).sum())
        fixed = max(1, used // 4)
        shifted = fixed + (places - fixed + offset_by * (used - fixed)) % max(1, number_of - fixed)
        return jnp.zeros((number_of,), jnp.int32).at[ranking[jnp.where(places < fixed, places, shifted)]].set(jnp.asarray(tallies, jnp.int32))

    tallies = jnp.where(number % 4 == 0, named(packed, number // 4), named(usual, number - number // 4 - 1))
    mixed = jax.random.permutation(jax.random.fold_in(own, 3), number_of)
    source_of, taker = mixed[0:number_of // 2 * 2:2], mixed[1:number_of // 2 * 2:2]
    slack = jnp.minimum(tallies[source_of] - 1, most - tallies[taker]) // 2
    slack = jnp.where((source_of == ranking[0]) | (taker == ranking[0]) | (tallies[taker] == 0), 0, jnp.maximum(slack, 0))
    shifted = jax.random.randint(jax.random.fold_in(own, 4), (number_of // 2,), 0, 1 << 20) % (slack + 1)
    tallies = tallies.at[source_of].add(-shifted).at[taker].add(shifted)
    items = jnp.searchsorted(jnp.cumsum(tallies), jnp.arange(rows * top), side="right").astype(jnp.int32)
    listing = items.reshape(top, rows).T
    listing = listing[jax.random.permutation(jax.random.fold_in(own, 1), rows)]
    offset_by = jax.random.randint(jax.random.fold_in(own, 2), (rows, 1), 0, top)
    return jnp.take_along_axis(listing, (jnp.arange(top)[None, :] + offset_by) % top, axis=1)


def shares(count, total, most, slope, full):
    loads = [(1 << 20) // math.isqrt(standing ** slope) + 1 for standing in range(1, count + 1)]
    largest = most if full else min(most, max(-(-total // count), total * loads[0] // sum(loads)))
    least = 1 if total - largest >= count - 1 else 0
    given, spare = [largest] + [least] * (count - 1), total - largest - least * (count - 1)
    while spare > 0:
        candidates = [i for i in range(1, count) if given[i] < largest] or [i for i in range(1, count) if given[i] < most]
        whole, remaining = sum([loads[i] for i in candidates]), spare
        for i in candidates:
            more = min(most - given[i], max(1, remaining * loads[i] // whole), spare)
            given[i] = given[i] + more
            spare = spare - more
    return np.array(given)


def bell_draw(own_key, extent, spread, reach, cuts=(), kind=jnp.bfloat16):
    values = spread * jax.random.normal(own_key, extent, jnp.float32)
    if cuts:
        values = values * level_of(own_key, extent, cuts, -0.22, 0.18)
    return jnp.clip(values, -reach, reach).astype(kind)


def setup_inputs(seed: int = 0) -> dict:
    key_list = jax.random.split(jax.random.key(seed), 20)
    q_latent = bell_draw(key_list[0], (TOKENS, QLAT), 1.0, 6.0, ((0, 128),))
    kv_latent = draw_kv_latent(jax.random.fold_in(key_list[19], 71), 0)
    rope_key = draw_rope_key(jax.random.fold_in(key_list[19], 71), 0)
    gain_query = jnp.clip(1.0 + 0.18 * jax.random.normal(key_list[3], (QLAT,), jnp.float32), 0.1, 1.9)
    gain_latent = jnp.clip(1.0 + 0.18 * jax.random.normal(key_list[4], (KVLAT,), jnp.float32), 0.1, 1.9)
    w_query = bell_draw(key_list[5], (QLAT, HEADS * (NOPE + ROPE)), QLAT ** -0.5, 0.1875, ((1, 4),))
    w_key = bell_draw(key_list[6], (KVLAT, HEADS * NOPE), (KVLAT // 6) ** -0.5, 0.625, ((1, 4),))
    w_value = bell_draw(key_list[7], (KVLAT, HEADS * VDIM), KVLAT ** -0.5, 0.25, ((1, 4),))
    w_out = bell_draw(key_list[8], (HEADS * VDIM, D), (HEADS * VDIM // 4) ** -0.5, 0.25, ((0, 4),))
    tokens_b = bell_draw(key_list[9], (TOKENS, D), 1.0, 6.0, ((0, 128),))
    gain_norm = jnp.clip(1.0 + 0.18 * jax.random.normal(key_list[10], (D,), jnp.float32), 0.1, 1.9)
    routes_keys = jax.random.split(jax.random.fold_in(key_list[11], 1), TOKENS // TOK_DEV)
    routes_turns = jax.random.permutation(jax.random.fold_in(key_list[11], 3), TOKENS // TOK_DEV)
    routes = jax.vmap(lambda own, number: shared_out(jax.random.fold_in(key_list[11], 2), own, number, TOK_DEV, EXPERTS, TOP_K, CAPQ, 1))(routes_keys, routes_turns).reshape((TOKENS, TOP_K))
    route_weights = jnp.clip(jnp.exp(math.log(1.0) - 1.609438 * jax.random.uniform(key_list[12], (TOKENS, TOP_K), jnp.float32) ** level_of(key_list[12], (TOKENS, TOP_K), ((0, 128),), -0.2, 0.2)), 0.2, 1.0)
    shared_gate = bell_draw(key_list[13], (D, FF), D ** -0.5, 0.09375, ((1, 4),))
    shared_up = bell_draw(key_list[14], (D, FF), D ** -0.5, 0.09375, ((1, 4),))
    shared_down = bell_draw(key_list[15], (FF, D), FF ** -0.5, 0.1875, ((0, 4),))
    expert_gate = bell_draw(key_list[16], (EXPERTS, D, FF), D ** -0.5, 0.09375, ((0, 32), (2, 4)))
    expert_up = bell_draw(key_list[17], (EXPERTS, D, FF), D ** -0.5, 0.09375, ((0, 32), (2, 4)))
    expert_down = bell_draw(key_list[18], (EXPERTS, FF, D), FF ** -0.5, 0.1875, ((0, 32), (1, 4)))
    return dict(q_latent=q_latent, kv_latent=kv_latent, rope_key=rope_key, gain_query=gain_query, gain_latent=gain_latent, w_query=w_query, w_key=w_key, w_value=w_value, w_out=w_out, tokens_b=tokens_b, gain_norm=gain_norm, routes=routes, route_weights=route_weights, shared_gate=shared_gate, shared_up=shared_up, shared_down=shared_down, expert_gate=expert_gate, expert_up=expert_up, expert_down=expert_down)


epsilon = 1e-06
rope_theta = 10000.0

def rms_scale(values, gain_vec):
    floats = values.astype(jnp.float32)
    scaled = floats * lax.rsqrt(lax.optimization_barrier(jnp.mean(floats * floats, axis=-1, keepdims=True)) + epsilon)
    return (scaled * gain_vec).astype(jnp.bfloat16)

def rope_angles(positions, rope_width):
    frequency = rope_theta ** (-jnp.arange(0, rope_width, 2, dtype=jnp.float32) / rope_width)
    angles = positions.astype(jnp.float32)[:, None] * frequency[None, :]
    return (jnp.cos(angles), jnp.sin(angles))

def rotate_pairs(values, cos_tab, sin_tab):
    half_width = values.shape[-1] // 2
    first_half = values[..., :half_width]
    second_half = values[..., half_width:]
    return jnp.concatenate([first_half * cos_tab - second_half * sin_tab, second_half * cos_tab + first_half * sin_tab], axis=-1)

def rounded(values):
    return lax.optimization_barrier(values.astype(jnp.bfloat16)).astype(jnp.float32)

def group_sum(hidden, down_weight):
    row_total = hidden.shape[0]
    hidden_groups = hidden.reshape(row_total, N_TP, -1)
    down_groups = down_weight.reshape(N_TP, -1, down_weight.shape[-1])
    running_sum = jnp.zeros((row_total, down_weight.shape[-1]), jnp.float32)
    for group_num in range(N_TP):
        partial_value = jnp.dot(hidden_groups[:, group_num], down_groups[group_num], preferred_element_type=jnp.float32)
        running_sum = running_sum + rounded(partial_value)
    return running_sum.astype(jnp.bfloat16)

def reference(q_latent, kv_latent, rope_key, gain_query, gain_latent, w_query, w_key, w_value, w_out, tokens_b, gain_norm, routes, route_weights, shared_gate, shared_up, shared_down, expert_gate, expert_up, expert_down):
    q_normed = rms_scale(q_latent, gain_query)
    kv_normed = rms_scale(kv_latent, gain_latent)
    positions = jnp.arange(TOKENS, dtype=jnp.int32) % LENGTH
    cos_tab, sin_tab = rope_angles(positions, ROPE)
    query_full = jnp.dot(q_normed, w_query, preferred_element_type=jnp.float32).reshape(TOKENS, HEADS, NOPE + ROPE)
    query_rot = rotate_pairs(query_full[:, :, NOPE:], cos_tab[:, None, :], sin_tab[:, None, :])
    queries = jnp.concatenate([query_full[:, :, :NOPE], query_rot], axis=-1).astype(jnp.bfloat16)
    rot_keys = rotate_pairs(rope_key.astype(jnp.float32), cos_tab, sin_tab).astype(jnp.bfloat16)
    keys = jnp.dot(kv_normed, w_key, preferred_element_type=jnp.float32).astype(jnp.bfloat16).reshape(TOKENS, HEADS, NOPE)
    values = jnp.dot(kv_normed, w_value, preferred_element_type=jnp.float32).astype(jnp.bfloat16).reshape(TOKENS, HEADS, VDIM)
    block_rows = TOK_DEV * N_TP
    block_count = TOKENS // block_rows

    def attend_block(block_num):
        first_row = (block_num * block_rows).astype(jnp.int32)
        seq_first = (first_row // LENGTH * LENGTH).astype(jnp.int32)
        query_blk = lax.dynamic_slice_in_dim(queries, first_row, block_rows, 0).astype(jnp.float32)
        key_blk = lax.dynamic_slice_in_dim(keys, seq_first, LENGTH, 0).astype(jnp.float32)
        pe_blk = lax.dynamic_slice_in_dim(rot_keys, seq_first, LENGTH, 0).astype(jnp.float32)
        value_blk = lax.dynamic_slice_in_dim(values, seq_first, LENGTH, 0).astype(jnp.float32)
        scores = jnp.einsum('qhd,khd->hqk', query_blk[:, :, :NOPE], key_blk)
        scores = scores + jnp.einsum('qhr,kr->hqk', query_blk[:, :, NOPE:], pe_blk)
        scores = scores * (NOPE + ROPE) ** (-0.5)
        query_pos = first_row + jnp.arange(block_rows, dtype=jnp.int32)
        key_pos = seq_first + jnp.arange(LENGTH, dtype=jnp.int32)
        allowed = key_pos[None, :] <= query_pos[:, None]
        scores = jnp.where(allowed[None], scores, -jnp.inf)
        row_top = lax.optimization_barrier(jnp.max(scores, axis=-1, keepdims=True))
        exp_terms = jnp.exp(scores - row_top)
        denom_sum = lax.optimization_barrier(jnp.sum(exp_terms, axis=-1))
        weights = rounded(exp_terms)
        weighted = jnp.einsum('hqk,khd->qhd', weights, value_blk)
        return (weighted / denom_sum.T[:, :, None]).astype(jnp.bfloat16)
    heads_out = lax.map(attend_block, jnp.arange(block_count, dtype=jnp.int32)).reshape(TOKENS, HEADS * VDIM)
    mixer_out = group_sum(heads_out, w_out)
    normed_b = rms_scale(tokens_b, gain_norm)
    block_total = TOKENS // TOK_DEV
    pair_ids = routes.reshape(block_total, TOK_DEV * TOP_K).astype(jnp.int32)
    onehot = (pair_ids[:, :, None] == jnp.arange(EXPERTS, dtype=jnp.int32)[None, None, :]).astype(jnp.int32)
    slot_ids = lax.optimization_barrier(jnp.sum((jnp.cumsum(onehot, axis=1) - onehot) * onehot, axis=-1)).astype(jnp.int32)
    token_ids = jnp.repeat(jnp.arange(TOKENS, dtype=jnp.int32).reshape(block_total, TOK_DEV), TOP_K, axis=1)
    block_ids = jnp.broadcast_to(jnp.arange(block_total, dtype=jnp.int32)[:, None], pair_ids.shape)
    slot_table = jnp.full((EXPERTS, block_total, CAPQ), TOKENS, jnp.int32).at[pair_ids, block_ids, slot_ids].set(token_ids)
    padded = jnp.concatenate([normed_b, jnp.zeros((1, D), jnp.bfloat16)], axis=0)

    def run_expert(expert_num):
        chosen = jnp.take(padded, slot_table[expert_num].reshape(-1), axis=0)
        gate_act = jnp.dot(chosen, expert_gate[expert_num], preferred_element_type=jnp.float32)
        up_act = jnp.dot(chosen, expert_up[expert_num], preferred_element_type=jnp.float32)
        hidden = (jax.nn.silu(gate_act) * up_act).astype(jnp.bfloat16)
        return group_sum(hidden, expert_down[expert_num])
    expert_rows = lax.map(run_expert, jnp.arange(EXPERTS, dtype=jnp.int32))
    flat_index = (pair_ids * (block_total * CAPQ) + block_ids * CAPQ + slot_ids).reshape(-1).astype(jnp.int32)
    picked = jnp.take(expert_rows.reshape(-1, D), flat_index, axis=0).reshape(TOKENS, TOP_K, D)
    gate_shared = jnp.dot(normed_b, shared_gate, preferred_element_type=jnp.float32)
    up_shared = jnp.dot(normed_b, shared_up, preferred_element_type=jnp.float32)
    shared_hidden = (jax.nn.silu(gate_shared) * up_shared).astype(jnp.bfloat16)
    shared_result = group_sum(shared_hidden, shared_down)
    routed_sum = lax.optimization_barrier(jnp.sum(route_weights[:, :, None] * picked.astype(jnp.float32), axis=1))
    expert_mix = (shared_result.astype(jnp.float32) + routed_sum).astype(jnp.bfloat16)
    return (mixer_out, expert_mix)
```

```python
import functools

import jax
import jax.numpy as jnp
import numpy as np
from jax import lax
from jax.experimental import pallas as pl
from jax.experimental.pallas import tpu as pltpu
from jax.sharding import Mesh
from jax.sharding import PartitionSpec as P

NOPE = 128
ROPE = 64
VDIM = 128
HEADS_DEV = 4
EP = ("ep_0", "ep_1", "ep_2")
EP_TP = ("ep_0", "ep_1", "ep_2", "tp")
N_EP = 32
N_TP = 4
ROWS = 128
GROUP = 512
WIDTH = 4096
CAP = 10
CHUNKS = 4
CHUNK = WIDTH // CHUNKS
WIRE = CAP * CHUNKS
SLOTS = N_EP * CAP
HALF = SLOTS // 2
PACKED = GROUP + ROPE
CALLS = 4
FORWARD_AFTER = 2

epsilon = 1e-06
rope_theta = 10000.0
bf16 = jnp.bfloat16
f32 = jnp.float32
i32 = jnp.int32


def whole(shape, dtype=bf16):
    return jax.ShapeDtypeStruct(shape, dtype)


def kernel_call(body, out_shape, flops=1000000, **kw):
    return pl.pallas_call(
        body,
        out_shape=out_shape,
        cost_estimate=pl.CostEstimate(flops=int(flops), bytes_accessed=1000000, transcendentals=0),
        **kw,
    )


def ring(steps):
    return [(i, (i + steps) % N_TP) for i in range(N_TP)]


def up(x):
    return lax.ppermute(x, "tp", ring(1))


def down(x):
    return lax.ppermute(x, "tp", ring(N_TP - 1))


def after(x, *deps):
    return lax.optimization_barrier((x, deps))[0]


def rope_angles(positions, rope_width):
    frequency = rope_theta ** (-jnp.arange(0, rope_width, 2, dtype=f32) / rope_width)
    angles = positions.astype(f32)[:, None] * frequency[None, :]
    return (jnp.cos(angles), jnp.sin(angles))


def rotate_pairs(values, cos_tab, sin_tab):
    half_width = values.shape[-1] // 2
    a = values[..., :half_width]
    b = values[..., half_width:]
    return jnp.concatenate([a * cos_tab - b * sin_tab, b * cos_tab + a * sin_tab], axis=-1)


def regroup_matrix():
    out = np.zeros((8 * WIRE, 8 * WIRE), np.float32)
    for c in range(CHUNKS):
        for s in range(8):
            for k in range(CAP):
                out[c * 8 * CAP + s * CAP + k, s * WIRE + c * CAP + k] = 1
    return out


def dispatch_body(tok_ref, gain_ref, routes_ref, norm_ref, wire_ref):
    x = tok_ref[...].astype(f32)
    mean = jnp.mean(x * x, axis=-1, keepdims=True)
    normed = ((x * lax.rsqrt(mean + epsilon)) * gain_ref[...]).astype(bf16)
    norm_ref[...] = normed
    r0 = routes_ref[0:1, :]
    r1 = routes_ref[1:2, :]
    expert = lax.broadcasted_iota(i32, (N_EP, ROWS), 0)
    hot0 = jnp.where(expert == r0, 1.0, 0.0)
    hot1 = jnp.where(expert == r1, 1.0, 0.0)
    before = lax.broadcasted_iota(i32, (ROWS, ROWS), 0) < lax.broadcasted_iota(i32, (ROWS, ROWS), 1)
    before = jnp.where(before, 1.0, 0.0).astype(bf16)
    seen0 = jnp.dot(hot0.astype(bf16), before, preferred_element_type=f32)
    seen1 = jnp.dot(hot1.astype(bf16), before, preferred_element_type=f32)
    seen1 = seen1 + jnp.sum(hot0, axis=1, keepdims=True)
    slot0 = jnp.sum(seen0 * hot0, axis=0, keepdims=True).astype(i32) + r0 * WIRE
    slot1 = jnp.sum(seen1 * hot1, axis=0, keepdims=True).astype(i32) + r1 * WIRE
    row = lax.broadcasted_iota(i32, (N_EP * WIRE, ROWS), 0)
    picks = jnp.concatenate(
        [
            jnp.where((row == slot0 + c * CAP) | (row == slot1 + c * CAP), 1.0, 0.0).astype(bf16)
            for c in range(CHUNKS)
        ],
        axis=1,
    )
    stacked = jnp.concatenate([normed[:, c * CHUNK : (c + 1) * CHUNK] for c in range(CHUNKS)], axis=0)
    wire_ref[...] = jnp.dot(picks, stacked, preferred_element_type=f32).astype(bf16)


def unwire_body(wire_ref, mat_ref, lo_ref, hi_ref):
    mat = mat_ref[...]
    for g in range(4):
        got = jnp.dot(mat, wire_ref[g * 8 * WIRE : (g + 1) * 8 * WIRE, :], preferred_element_type=f32)
        got = got.astype(bf16)
        out_ref = lo_ref if g < 2 else hi_ref
        base = (g % 2) * 8 * CAP
        for c in range(CHUNKS):
            out_ref[base : base + 8 * CAP, c * CHUNK : (c + 1) * CHUNK] = got[c * 8 * CAP : (c + 1) * 8 * CAP, :]


def rewire_body(ol, oh, ml, mh, pl_, ph, mat_ref, wire_ref):
    mat = mat_ref[...]
    for g in range(4):
        own, fm, fp = (ol, ml, pl_) if g < 2 else (oh, mh, ph)
        base = (g % 2) * 8 * CAP
        pieces = []
        for c in range(CHUNKS):
            sl = (slice(base, base + 8 * CAP), slice(c * CHUNK, (c + 1) * CHUNK))
            total = own[sl].astype(f32) + fm[sl].astype(f32) + fp[sl].astype(f32)
            pieces.append(total.astype(bf16))
        rows = jnp.concatenate(pieces, axis=0)
        got = jnp.dot(mat, rows, preferred_element_type=f32)
        wire_ref[g * 8 * WIRE : (g + 1) * 8 * WIRE, :] = got.astype(bf16)


def ffn_body(*refs):
    count = (len(refs) - 3) // 2
    xs, (gate, upw, downw), outs = refs[:count], refs[count : count + 3], refs[count + 3 :]
    for x_ref, out_ref in zip(xs, outs):
        x = x_ref[...]
        g = jnp.dot(x, gate[...], preferred_element_type=f32)
        u = jnp.dot(x, upw[...], preferred_element_type=f32)
        hidden = ((g / (1.0 + jnp.exp(-g))) * u).astype(bf16)
        out_ref[...] = jnp.dot(hidden, downw[...], preferred_element_type=f32).astype(bf16)


def ffn(xs, gate, upw, downw):
    rows = sum(x.shape[0] for x in xs)
    call = kernel_call(ffn_body, tuple(whole(x.shape) for x in xs), flops=rows * WIDTH * 256 * 6)
    return call(*xs, gate, upw, downw)


def combine_body(ret_ref, routes_ref, rw_ref, own, ml, mh, pl_, ph, out_ref):
    r0 = routes_ref[:, 0:1]
    r1 = routes_ref[:, 1:2]
    expert = lax.broadcasted_iota(i32, (ROWS, N_EP), 1)
    hot0 = jnp.where(expert == r0, 1.0, 0.0)
    hot1 = jnp.where(expert == r1, 1.0, 0.0)
    before = lax.broadcasted_iota(i32, (ROWS, ROWS), 1) < lax.broadcasted_iota(i32, (ROWS, ROWS), 0)
    before = jnp.where(before, 1.0, 0.0).astype(bf16)
    seen0 = jnp.dot(before, hot0.astype(bf16), preferred_element_type=f32)
    seen1 = jnp.dot(before, hot1.astype(bf16), preferred_element_type=f32)
    seen1 = seen1 + jnp.sum(hot0, axis=0, keepdims=True)
    slot0 = jnp.sum(seen0 * hot0, axis=1, keepdims=True).astype(i32) + r0 * WIRE
    slot1 = jnp.sum(seen1 * hot1, axis=1, keepdims=True).astype(i32) + r1 * WIRE
    col = lax.broadcasted_iota(i32, (ROWS, N_EP * WIRE), 1)
    w0 = rw_ref[:, 0:1]
    w1 = rw_ref[:, 1:2]
    ret = ret_ref[...]
    for c in range(CHUNKS):
        picks = jnp.concatenate(
            [
                jnp.where(col == slot0 + c * CAP, 1.0, 0.0).astype(bf16),
                jnp.where(col == slot1 + c * CAP, 1.0, 0.0).astype(bf16),
            ],
            axis=0,
        )
        got = jnp.dot(picks, ret, preferred_element_type=f32)
        routed = w0 * got[:ROWS] + w1 * got[ROWS:]
        cols = slice(c * CHUNK, (c + 1) * CHUNK)
        for h, fm, fp in ((0, ml, pl_), (1, mh, ph)):
            rows = slice(h * 64, h * 64 + 64)
            shared = own[rows, cols].astype(f32) + fm[:, cols].astype(f32) + fp[:, cols].astype(f32)
            shared = shared.astype(bf16).astype(f32)
            out_ref[rows, cols] = (shared + routed[h * 64 : h * 64 + 64]).astype(bf16)


def prep_body(q_ref, kv_ref, rot_ref, gq_ref, gkv_ref, out_ref):
    def norm(ref, gain):
        x = ref[...].astype(f32)
        mean = jnp.mean(x * x, axis=-1, keepdims=True)
        return ((x * lax.rsqrt(mean + epsilon)) * gain[...]).astype(bf16)

    out_ref[0:ROWS, :] = norm(q_ref, gq_ref)
    kv = norm(kv_ref, gkv_ref)
    out_ref[ROWS : ROWS + 64, 0:512] = kv[:64]
    out_ref[ROWS : ROWS + 64, 512:1024] = kv[64:]
    out_ref[ROWS + 64 : ROWS + 72, :] = rot_ref[...]


def attend_body(first, last, base, blocks, rank_ref, q_ref, lat_ref, wk_ref, wv_ref, *refs):
    if first:
        state_in = None
    else:
        state_in, refs = refs[:3], refs[3:]
    if last:
        out_ref, refs = refs[0], refs[1:]
        kcat, val, m_ref, l_ref, acc_ref = refs
    else:
        m_out, l_out, acc_out = refs[:3]
        kcat, val, m_ref, l_ref, acc_ref = refs[3:]
    step = pl.program_id(0)
    rank = rank_ref[0]
    block = step + base

    @pl.when(step == 0)
    def _():
        if first:
            m_ref[...] = jnp.full(m_ref.shape, -jnp.inf, f32)
            l_ref[...] = jnp.zeros(l_ref.shape, f32)
            acc_ref[...] = jnp.zeros(acc_ref.shape, f32)
        else:
            m_ref[...] = state_in[0][...]
            l_ref[...] = state_in[1][...]
            acc_ref[...] = state_in[2][...]

    def work(diagonal):
        kv = lat_ref[0:GROUP, :]
        keys = jnp.dot(kv, wk_ref[...], preferred_element_type=f32).astype(bf16)
        val[...] = jnp.dot(kv, wv_ref[...], preferred_element_type=f32).astype(bf16)
        low = lax.broadcasted_iota(i32, (ROPE, 128), 1) < ROPE
        zero = jnp.zeros((ROPE, 128), bf16)
        rots = []
        for i in range(4):
            pair = lat_ref[GROUP : GROUP + ROPE, i * 128 : (i + 1) * 128]
            rots += [jnp.where(low, pair, zero), jnp.where(low, zero, pair)]
        rot = jnp.concatenate(rots, axis=0)
        for h in range(HEADS_DEV):
            kcat[:, h * 256 : h * 256 + 128] = keys[:, h * 128 : (h + 1) * 128]
            kcat[:, h * 256 + 128 : (h + 1) * 256] = rot
        scale = (NOPE + ROPE) ** (-0.5) * 1.4426950408889634

        def score(h):
            return lax.dot_general(
                q_ref[:, h * 256 : (h + 1) * 256],
                kcat[:, h * 256 : (h + 1) * 256],
                (((1,), (1,)), ((), ())),
                preferred_element_type=f32,
            )

        ahead = score(0)
        for h in range(HEADS_DEV):
            scores = ahead
            if h + 1 < HEADS_DEV:
                ahead = score(h + 1)
            if diagonal:
                row_id = lax.broadcasted_iota(i32, (GROUP, GROUP), 0)
                col_id = lax.broadcasted_iota(i32, (GROUP, GROUP), 1)
                scores = jnp.where(row_id >= col_id, scores, -jnp.inf)
            m_old = m_ref[h]
            m_new = jnp.maximum(m_old, jnp.max(scores, axis=-1, keepdims=True))
            factor = jnp.exp2((m_old - m_new) * scale)
            wide = jnp.concatenate([m_new] * 4, axis=1)
            terms = jnp.exp2((scores - wide) * scale)
            part = (terms[:, 0:128] + terms[:, 128:256]) + (terms[:, 256:384] + terms[:, 384:512])
            m_ref[h] = m_new
            l_ref[h] = l_ref[h] * factor + part
            update = jnp.dot(
                terms.astype(bf16), val[:, h * 128 : (h + 1) * 128], preferred_element_type=f32
            )
            acc_ref[h] = acc_ref[h] * factor + update

    @pl.when(block < rank)
    def _():
        work(False)

    @pl.when(block == rank)
    def _():
        work(True)

    @pl.when(step == blocks - 1)
    def _():
        if last:
            for h in range(HEADS_DEV):
                total = jnp.sum(l_ref[h], axis=-1, keepdims=True)
                out_ref[:, h * 128 : (h + 1) * 128] = (acc_ref[h] / total).astype(bf16)
        else:
            m_out[...] = m_ref[...]
            l_out[...] = l_ref[...]
            acc_out[...] = acc_ref[...]


def attend(call_num, rank, q, latents, w_key, w_value, state):
    blocks = N_EP // CALLS
    base = call_num * blocks
    first = call_num == 0
    last = call_num == CALLS - 1
    state_shape = (HEADS_DEV, GROUP, 128)
    same2 = lambda i, r: (0, 0)
    same3 = lambda i, r: (0, 0, 0)
    in_specs = [
        pl.BlockSpec((GROUP, HEADS_DEV * 256), same2),
        pl.BlockSpec((PACKED, GROUP), lambda i, r: (jnp.minimum(i + base, r[0]), 0)),
        pl.BlockSpec((512, 512), same2),
        pl.BlockSpec((512, 512), same2),
    ]
    args = [q, latents, w_key, w_value]
    if not first:
        in_specs += [pl.BlockSpec(state_shape, same3)] * 3
        args += list(state)
    if last:
        out_shape = whole((GROUP, HEADS_DEV * VDIM))
        out_specs = pl.BlockSpec((GROUP, HEADS_DEV * VDIM), same2)
    else:
        out_shape = (whole(state_shape, f32),) * 3
        out_specs = (pl.BlockSpec(state_shape, same3),) * 3
    return pl.pallas_call(
        functools.partial(attend_body, first, last, base, blocks),
        out_shape=out_shape,
        grid_spec=pltpu.PrefetchScalarGridSpec(
            num_scalar_prefetch=1,
            grid=(blocks,),
            in_specs=in_specs,
            out_specs=out_specs,
            scratch_shapes=[
                pltpu.VMEM((GROUP, HEADS_DEV * 256), bf16),
                pltpu.VMEM((GROUP, HEADS_DEV * VDIM), bf16),
                pltpu.VMEM(state_shape, f32),
                pltpu.VMEM(state_shape, f32),
                pltpu.VMEM(state_shape, f32),
            ],
        ),
        compiler_params=pltpu.CompilerParams(dimension_semantics=("arbitrary",)),
        cost_estimate=pl.CostEstimate(
            flops=int(blocks * 1.4e9), bytes_accessed=10000000, transcendentals=0
        ),
    )(rank, *args)


def on_device(
    q_latent,
    kv_latent,
    rope_key,
    gain_query,
    gain_latent,
    w_query,
    w_key,
    w_value,
    w_out,
    tokens_b,
    gain_norm,
    routes,
    route_weights,
    shared_gate,
    shared_up,
    shared_down,
    expert_gate,
    expert_up,
    expert_down,
):
    rank = lax.axis_index(EP)
    tp_rank = lax.axis_index("tp")
    regroup = jnp.asarray(regroup_matrix(), bf16)
    regroup_back = jnp.asarray(regroup_matrix().T, bf16)
    expert_gate, expert_up, expert_down = expert_gate[0], expert_up[0], expert_down[0]

    normed, wire = kernel_call(
        dispatch_body, (whole((ROWS, WIDTH)), whole((N_EP * WIRE, CHUNK))), flops=2e9
    )(tokens_b, gain_norm.reshape(1, WIDTH), routes.T)
    s_lo, s_hi = normed[:64], normed[64:]
    sm_lo, sp_hi = up(s_lo), down(s_hi)
    sm_hi, sp_lo = up(s_hi), down(s_lo)
    arrived = lax.all_to_all(wire.reshape(N_EP, WIRE, CHUNK), EP, 0, 0, tiled=True)
    x_lo, x_hi = kernel_call(unwire_body, (whole((HALF, WIDTH)),) * 2, flops=2e9)(
        arrived.reshape(N_EP * WIRE, CHUNK), regroup
    )

    positions = rank * GROUP + jnp.arange(GROUP, dtype=i32)
    cos_tab, sin_tab = rope_angles(positions, ROPE)
    own_cos, own_sin = rope_angles(
        rank * GROUP + tp_rank * ROWS + jnp.arange(ROWS, dtype=i32), ROPE
    )
    rot_key = rotate_pairs(rope_key.astype(f32), own_cos, own_sin).astype(bf16)
    rot_pair = jnp.concatenate([rot_key[:64], rot_key[64:]], axis=1)
    rot_rows = jnp.concatenate([rot_pair[8 * g : 8 * g + 8] for g in range(8)], axis=1)
    pack = kernel_call(prep_body, whole((200, 1024)), flops=1e6)(
        q_latent, kv_latent, rot_rows, gain_query.reshape(1, -1), gain_latent.reshape(1, -1)
    )
    packs = lax.all_gather(pack, "tp", axis=0, tiled=False)
    kv_part = packs[:, ROWS : ROWS + 64]
    kv_rows = jnp.concatenate(
        [kv_part[t, :, h * 512 : (h + 1) * 512] for t in range(N_TP) for h in range(2)], axis=0
    )
    rot_part = packs[:, ROWS + 64 :]
    rot_rows = jnp.concatenate(
        [
            jnp.concatenate([rot_part[t, :, g * 128 : (g + 1) * 128] for g in range(8)], axis=0)
            for t in range(N_TP)
        ],
        axis=1,
    )
    latents = jnp.concatenate([kv_rows, rot_rows], axis=0)
    latents = lax.all_gather(latents, EP, axis=0, tiled=True)

    s2_lo, s2_hi = up(sm_lo), down(sp_hi)
    m_lo, p_hi = up(x_lo), down(x_hi)
    m_hi, p_lo = up(x_hi), down(x_lo)
    t_lo, t_hi = up(m_lo), down(p_hi)

    shared_w = (shared_gate, shared_up, shared_down)
    routed_w = (expert_gate, expert_up, expert_down)
    (own_s,) = ffn((after(normed, x_lo),), *shared_w)

    query_in = after(packs[:, :ROWS].reshape(GROUP, 1024), own_s)
    query_full = jnp.dot(query_in, w_query, preferred_element_type=f32)
    query_full = query_full.reshape(GROUP, HEADS_DEV, NOPE + ROPE)
    query_rot = rotate_pairs(
        query_full[:, :, NOPE:], cos_tab[:, None, :], sin_tab[:, None, :]
    ).astype(bf16)
    query_nope = query_full[:, :, :NOPE].astype(bf16)
    queries = jnp.concatenate([query_nope, query_rot, query_rot], axis=-1).reshape(GROUP, -1)

    own_lo, own_hi = ffn((after(x_lo, queries), x_hi), *routed_w)
    ms_lo, ms_hi, ps_lo, ps_hi = ffn((after(sm_lo, own_lo), sm_hi, sp_lo, sp_hi), *shared_w)
    ts_lo, ts_hi = ffn((after(s2_lo, ms_lo), s2_hi), *shared_w)
    mr_lo, mr_hi, pr_lo, pr_hi = ffn((after(m_lo, ts_lo), m_hi, p_lo, p_hi), *routed_w)
    tr_lo, tr_hi = ffn((after(t_lo, mr_lo), t_hi), *routed_w)

    def add(a, b):
        return (a.astype(f32) + b.astype(f32)).astype(bf16)

    fm_hi, fp_lo = up(pr_hi), down(mr_lo)
    via_lo, via_hi = up(tr_lo), down(tr_hi)
    svia_lo, svia_hi = up(ts_lo), down(ts_hi)
    sfm_hi, sfp_lo = up(ps_hi), down(ms_lo)

    rank_arr = jnp.full((1,), rank, i32)
    state = None
    states = []
    queries = after(queries, tr_lo)
    for call_num in range(CALLS):
        state = attend(call_num, rank_arr, queries, latents, w_key, w_value, state)
        states.append(state)

    ready = states[FORWARD_AFTER][1]
    via_lo, via_hi, svia_lo, svia_hi = lax.optimization_barrier(
        ((via_lo, via_hi, svia_lo, svia_hi), ready)
    )[0]
    fm_lo, fp_hi = up(add(pr_lo, via_lo)), down(add(mr_hi, via_hi))
    sfm_lo, sfp_hi = up(add(ps_lo, svia_lo)), down(add(ms_hi, svia_hi))

    back = kernel_call(rewire_body, whole((N_EP * WIRE, CHUNK)), flops=2e9)(
        own_lo, own_hi, fm_lo, fm_hi, fp_lo, fp_hi, regroup_back
    )
    returned = lax.all_to_all(back.reshape(N_EP, WIRE, CHUNK), EP, 0, 0, tiled=True)

    partial = jnp.dot(state, w_out, preferred_element_type=f32).astype(bf16)
    mixer_out = lax.psum_scatter(partial, "tp", scatter_dimension=0, tiled=True)

    expert_mix = kernel_call(combine_body, whole((ROWS, WIDTH)), flops=3e9)(
        returned.reshape(N_EP * WIRE, CHUNK),
        routes,
        route_weights,
        own_s,
        sfm_lo,
        sfm_hi,
        sfp_lo,
        sfp_hi,
    )
    return (mixer_out, expert_mix)


def solution(mesh):
    finer = Mesh(mesh.devices.reshape(4, 4, 2, mesh.shape["tp"]), ("ep_0", "ep_1", "ep_2", "tp"))
    placed = (
        P(EP_TP, None),
        P(EP_TP, None),
        P(EP_TP, None),
        P(),
        P(),
        P(None, "tp"),
        P(None, "tp"),
        P(None, "tp"),
        P("tp", None),
        P(EP_TP, None),
        P(),
        P(EP_TP, None),
        P(EP_TP, None),
        P(None, "tp"),
        P(None, "tp"),
        P("tp", None),
        P(EP, None, "tp"),
        P(EP, None, "tp"),
        P(EP, "tp", None),
    )
    return jax.shard_map(
        on_device,
        mesh=finer,
        in_specs=placed,
        out_specs=(P(EP_TP, None), P(EP_TP, None)),
        check_vma=False,
    )
```

```python
import functools

import jax
import jax.numpy as jnp
import numpy as np
from jax import lax
from jax.experimental import pallas as pl
from jax.experimental.pallas import tpu as pltpu
from jax.sharding import Mesh
from jax.sharding import PartitionSpec as P

NOPE = 128
ROPE = 64
VDIM = 128
HEADS_DEV = 4
EP = ("ep_0", "ep_1", "ep_2")
EP_TP = ("ep_0", "ep_1", "ep_2", "tp")
N_EP = 32
N_TP = 4
ROWS = 128
GROUP = 512
WIDTH = 4096
CAP = 10
CHUNKS = 4
CHUNK = WIDTH // CHUNKS
WIRE = CAP * CHUNKS
SLOTS = N_EP * CAP
HALF = SLOTS // 2
SCALE = (NOPE + ROPE) ** (-0.5) * 1.4426950408889634

epsilon = 1e-06
rope_theta = 10000.0
bf16 = jnp.bfloat16
f32 = jnp.float32
i32 = jnp.int32


def whole(shape, dtype=bf16):
    return jax.ShapeDtypeStruct(shape, dtype)


def kernel_call(body, out_shape, flops=1000000, **kw):
    return pl.pallas_call(
        body,
        out_shape=out_shape,
        cost_estimate=pl.CostEstimate(flops=int(flops), bytes_accessed=1000000, transcendentals=0),
        **kw,
    )


def ring(steps):
    return [(i, (i + steps) % N_TP) for i in range(N_TP)]


def up(x):
    return lax.ppermute(x, "tp", ring(1))


def down(x):
    return lax.ppermute(x, "tp", ring(N_TP - 1))


def after(x, *deps):
    return lax.optimization_barrier((x, deps))[0]


def rope_angles(positions, rope_width):
    frequency = rope_theta ** (-jnp.arange(0, rope_width, 2, dtype=f32) / rope_width)
    angles = positions.astype(f32)[:, None] * frequency[None, :]
    return (jnp.cos(angles), jnp.sin(angles))


def rotate_pairs(values, cos_tab, sin_tab):
    half_width = values.shape[-1] // 2
    a = values[..., :half_width]
    b = values[..., half_width:]
    return jnp.concatenate([a * cos_tab - b * sin_tab, b * cos_tab + a * sin_tab], axis=-1)


def regroup_matrix():
    out = np.zeros((8 * WIRE, 8 * WIRE), np.float32)
    for c in range(CHUNKS):
        for s in range(8):
            for k in range(CAP):
                out[c * 8 * CAP + s * CAP + k, s * WIRE + c * CAP + k] = 1
    return out


def place(normed, routes_ref):
    r0 = routes_ref[0:1, :]
    r1 = routes_ref[1:2, :]
    expert = lax.broadcasted_iota(i32, (N_EP, ROWS), 0)
    hot0 = jnp.where(expert == r0, 1.0, 0.0)
    hot1 = jnp.where(expert == r1, 1.0, 0.0)
    before = lax.broadcasted_iota(i32, (ROWS, ROWS), 0) < lax.broadcasted_iota(i32, (ROWS, ROWS), 1)
    before = jnp.where(before, 1.0, 0.0).astype(bf16)
    seen0 = jnp.dot(hot0.astype(bf16), before, preferred_element_type=f32)
    seen1 = jnp.dot(hot1.astype(bf16), before, preferred_element_type=f32)
    seen1 = seen1 + jnp.sum(hot0, axis=1, keepdims=True)
    slot0 = jnp.sum(seen0 * hot0, axis=0, keepdims=True).astype(i32) + r0 * WIRE
    slot1 = jnp.sum(seen1 * hot1, axis=0, keepdims=True).astype(i32) + r1 * WIRE
    row = lax.broadcasted_iota(i32, (N_EP * WIRE, ROWS), 0)
    picks = jnp.concatenate(
        [
            jnp.where((row == slot0 + c * CAP) | (row == slot1 + c * CAP), 1.0, 0.0).astype(bf16)
            for c in range(CHUNKS)
        ],
        axis=1,
    )
    stacked = jnp.concatenate([normed[:, c * CHUNK : (c + 1) * CHUNK] for c in range(CHUNKS)], axis=0)
    return jnp.dot(picks, stacked, preferred_element_type=f32).astype(bf16)


def dispatch_body(tok_ref, gain_ref, routes_ref, lo_ref, hi_ref, wire_ref):
    x = tok_ref[...].astype(f32)
    mean = jnp.mean(x * x, axis=-1, keepdims=True)
    normed = ((x * lax.rsqrt(mean + epsilon)) * gain_ref[...]).astype(bf16)
    lo_ref[...] = normed[:64]
    hi_ref[...] = normed[64:]
    wire_ref[...] = place(normed, routes_ref)


def dispatch_far_body(lo_ref, hi_ref, routes_ref, wire_ref):
    wire_ref[...] = place(jnp.concatenate([lo_ref[...], hi_ref[...]], axis=0), routes_ref)


def unwire_body(wire_ref, mat_ref, lo_ref, hi_ref):
    mat = mat_ref[...]
    for g in range(4):
        got = jnp.dot(mat, wire_ref[g * 8 * WIRE : (g + 1) * 8 * WIRE, :], preferred_element_type=f32)
        got = got.astype(bf16)
        out_ref = lo_ref if g < 2 else hi_ref
        base = (g % 2) * 8 * CAP
        for c in range(CHUNKS):
            out_ref[base : base + 8 * CAP, c * CHUNK : (c + 1) * CHUNK] = got[c * 8 * CAP : (c + 1) * 8 * CAP, :]


def rewire_body(*refs):
    parts, mat, wire_ref = refs[:-2], refs[-2][...], refs[-1]
    for g in range(4):
        base = (g % 2) * 8 * CAP
        pieces = []
        for c in range(CHUNKS):
            sl = (slice(base, base + 8 * CAP), slice(c * CHUNK, (c + 1) * CHUNK))
            terms = [part[sl] for part in parts[g // 2 :: 2]]
            if len(terms) == 1:
                pieces.append(terms[0])
            else:
                total = terms[0].astype(f32)
                for term in terms[1:]:
                    total = total + term.astype(f32)
                pieces.append(total.astype(bf16))
        rows = jnp.concatenate(pieces, axis=0)
        got = jnp.dot(mat, rows, preferred_element_type=f32)
        wire_ref[g * 8 * WIRE : (g + 1) * 8 * WIRE, :] = got.astype(bf16)


def ffn_body(*refs):
    count = (len(refs) - 3) // 2
    xs, (gate, upw, downw), outs = refs[:count], refs[count : count + 3], refs[count + 3 :]
    for x_ref, out_ref in zip(xs, outs):
        x = x_ref[...]
        g = jnp.dot(x, gate[...], preferred_element_type=f32)
        u = jnp.dot(x, upw[...], preferred_element_type=f32)
        hidden = ((g / (1.0 + jnp.exp(-g))) * u).astype(bf16)
        out_ref[...] = jnp.dot(hidden, downw[...], preferred_element_type=f32).astype(bf16)


def ffn(xs, gate, upw, downw):
    rows = sum(x.shape[0] for x in xs)
    call = kernel_call(ffn_body, tuple(whole(x.shape) for x in xs), flops=rows * WIDTH * 256 * 6)
    return call(*xs, gate, upw, downw)


def combine_body(count, *refs):
    ret_ref, routes_ref, rw_ref = refs[:3]
    shared, (lo_ref, hi_ref) = refs[3 : 3 + count], refs[3 + count :]
    r0 = routes_ref[:, 0:1]
    r1 = routes_ref[:, 1:2]
    expert = lax.broadcasted_iota(i32, (ROWS, N_EP), 1)
    hot0 = jnp.where(expert == r0, 1.0, 0.0)
    hot1 = jnp.where(expert == r1, 1.0, 0.0)
    before = lax.broadcasted_iota(i32, (ROWS, ROWS), 1) < lax.broadcasted_iota(i32, (ROWS, ROWS), 0)
    before = jnp.where(before, 1.0, 0.0).astype(bf16)
    seen0 = jnp.dot(before, hot0.astype(bf16), preferred_element_type=f32)
    seen1 = jnp.dot(before, hot1.astype(bf16), preferred_element_type=f32)
    seen1 = seen1 + jnp.sum(hot0, axis=0, keepdims=True)
    slot0 = jnp.sum(seen0 * hot0, axis=1, keepdims=True).astype(i32) + r0 * WIRE
    slot1 = jnp.sum(seen1 * hot1, axis=1, keepdims=True).astype(i32) + r1 * WIRE
    col = lax.broadcasted_iota(i32, (ROWS, N_EP * WIRE), 1)
    w0 = rw_ref[:, 0:1]
    w1 = rw_ref[:, 1:2]
    ret = ret_ref[...]
    for c in range(CHUNKS):
        picks = jnp.concatenate(
            [
                jnp.where(col == slot0 + c * CAP, 1.0, 0.0).astype(bf16),
                jnp.where(col == slot1 + c * CAP, 1.0, 0.0).astype(bf16),
            ],
            axis=0,
        )
        got = jnp.dot(picks, ret, preferred_element_type=f32)
        routed = w0 * got[:ROWS] + w1 * got[ROWS:]
        cols = slice(c * CHUNK, (c + 1) * CHUNK)
        for h, out_ref in ((0, lo_ref), (1, hi_ref)):
            total = routed[h * 64 : h * 64 + 64]
            for part in shared[h::2]:
                total = total + part[:, cols].astype(f32)
            if out_ref.shape[0] == ROWS:
                lo_ref[h * 64 : h * 64 + 64, cols] = total.astype(bf16)
            else:
                out_ref[:, cols] = total.astype(bf16)


def combine_whole_body(*refs):
    combine_body(6, *refs, refs[-1])


def sum_body(*refs):
    out_ref = refs[-1]
    for h in range(2):
        total = refs[h][...].astype(f32) + refs[2 + h][...].astype(f32) + refs[4 + h][...].astype(f32)
        out_ref[h * 64 : h * 64 + 64, :] = total.astype(bf16)


OUT_SPECS = [pl.BlockSpec(memory_space=pltpu.SMEM)] + [pl.BlockSpec(memory_space=pltpu.VMEM)] * 3


def out_body(heavy_ref, own_ref, other_ref, w_ref, *outs):
    heads = []
    for h in range(HEADS_DEV):
        cols = slice(h * 128, (h + 1) * 128)
        m_own, l_own = own_ref[:, 512 + h : 513 + h], own_ref[:, 516 + h : 517 + h]
        m_other, l_other = other_ref[:, 512 + h : 513 + h], other_ref[:, 516 + h : 517 + h]
        m_other = jnp.where(heavy_ref[0] > 0, m_other, -jnp.inf)
        top = jnp.maximum(m_own, m_other)
        f_own = jnp.exp2((m_own - top) * SCALE)
        f_other = jnp.exp2((m_other - top) * SCALE)
        total = l_own * f_own + l_other * f_other
        acc = own_ref[:, cols] * f_own + other_ref[:, cols] * f_other
        heads.append((acc / total).astype(bf16))
    got = jnp.dot(jnp.concatenate(heads, axis=1), w_ref[...], preferred_element_type=f32).astype(bf16)
    for k, out_ref in enumerate(outs):
        out_ref[...] = got[k * 64 : (k + 1) * 64]


def prep_body(q_ref, kv_ref, rot_ref, gq_ref, gkv_ref, *outs):
    def norm(ref, gain):
        x = ref[...].astype(f32)
        mean = jnp.mean(x * x, axis=-1, keepdims=True)
        return ((x * lax.rsqrt(mean + epsilon)) * gain[...]).astype(bf16)

    q_out, kv_out = outs
    q_out[...] = norm(q_ref, gq_ref)
    kv = norm(kv_ref, gkv_ref)
    kv_out[0:64, 0:512] = kv[:64]
    kv_out[0:64, 512:1024] = kv[64:]
    kv_out[64:72, :] = rot_ref[...]


def repack_body(*refs):
    out_ref = refs[-1]
    for j in range(N_TP):
        out_ref[j * 64 : (j + 1) * 64, :] = refs[j][0:64, :]
        rot = refs[j][64:72, :].astype(f32)
        for half in range(2):
            piece = [rot[:, g * 128 : (g + 1) * 128] for g in range(4 * half, 4 * half + 4)]
            g = 2 * j + half
            out_ref[256:288, g * 128 : (g + 1) * 128] = jnp.concatenate(piece, axis=0).astype(bf16)


def attend_body(plan_ref, q_ref, lat_ref, wk_ref, wv_ref, out_ref, kcat, val, m_ref, l_ref, acc_ref):
    step = pl.program_id(0)
    block = step + plan_ref[0]

    @pl.when(step == 0)
    def _():
        m_ref[...] = jnp.full(m_ref.shape, -jnp.inf, f32)
        l_ref[...] = jnp.zeros(l_ref.shape, f32)
        acc_ref[...] = jnp.zeros(acc_ref.shape, f32)

    def work(diagonal):
        low = lax.broadcasted_iota(i32, (256, 128), 1) < ROPE
        zero = jnp.zeros((256, 128), bf16)
        pair = jnp.concatenate([lat_ref[256:288, g * 128 : (g + 1) * 128] for g in range(8)], axis=0)
        for half in range(2):
            kv = lat_ref[0:256, half * 512 : half * 512 + 512]
            rows = slice(half * 256, half * 256 + 256)
            keys = jnp.dot(kv, wk_ref[...], preferred_element_type=f32).astype(bf16)
            val[rows, :] = jnp.dot(kv, wv_ref[...], preferred_element_type=f32).astype(bf16)
            rot = jnp.where(low, pair, zero) if half == 0 else jnp.where(low, zero, pair)
            for h in range(HEADS_DEV):
                kcat[rows, h * 256 : h * 256 + 128] = keys[:, h * 128 : (h + 1) * 128]
                kcat[rows, h * 256 + 128 : (h + 1) * 256] = rot

        def score(h):
            return lax.dot_general(
                q_ref[:, h * 256 : (h + 1) * 256],
                kcat[:, h * 256 : (h + 1) * 256],
                (((1,), (1,)), ((), ())),
                preferred_element_type=f32,
            )

        ahead = score(0)
        for h in range(HEADS_DEV):
            scores = ahead
            if h + 1 < HEADS_DEV:
                ahead = score(h + 1)
            if diagonal:
                row = lax.broadcasted_iota(i32, (GROUP, GROUP), 0)
                col = lax.broadcasted_iota(i32, (GROUP, GROUP), 1)
                row = ((plan_ref[3] - (row >> 7)) & 3) * 128 + (row & 127)
                piece = (plan_ref[3] - ((col & 255) >> 6)) & 3
                col = piece * 128 + (col >> 8) * 64 + (col & 63)
                scores = jnp.where(row >= col, scores, -jnp.inf)
            m_old = m_ref[h]
            m_new = jnp.maximum(m_old, jnp.max(scores, axis=-1, keepdims=True))
            factor = jnp.exp2((m_old - m_new) * SCALE)
            wide = jnp.concatenate([m_new] * 4, axis=1)
            terms = jnp.exp2((scores - wide) * SCALE)
            part = (terms[:, 0:128] + terms[:, 128:256]) + (terms[:, 256:384] + terms[:, 384:512])
            m_ref[h] = m_new
            l_ref[h] = l_ref[h] * factor + part
            update = jnp.dot(
                terms.astype(bf16), val[:, h * 128 : (h + 1) * 128], preferred_element_type=f32
            )
            acc_ref[h] = acc_ref[h] * factor + update

    @pl.when((step < plan_ref[1]) & (block != plan_ref[2]))
    def _():
        work(False)

    @pl.when((step < plan_ref[1]) & (block == plan_ref[2]))
    def _():
        work(True)

    @pl.when(step == pl.num_programs(0) - 1)
    def _():
        lane = lax.broadcasted_iota(i32, (GROUP, 128), 1)
        stats = jnp.zeros((GROUP, 128), f32)
        for h in range(HEADS_DEV):
            out_ref[:, h * 128 : (h + 1) * 128] = acc_ref[h]
            stats = jnp.where(lane == h, m_ref[h], stats)
            stats = jnp.where(lane == 4 + h, jnp.sum(l_ref[h], axis=-1, keepdims=True), stats)
        out_ref[:, 512:640] = stats


def attend(steps, plan, q, latents, w_key, w_value):
    state_shape = (HEADS_DEV, GROUP, 128)
    same = lambda i, r: (0, 0)
    return pl.pallas_call(
        attend_body,
        out_shape=whole((GROUP, 640), f32),
        grid_spec=pltpu.PrefetchScalarGridSpec(
            num_scalar_prefetch=1,
            grid=(steps,),
            in_specs=[
                pl.BlockSpec((GROUP, HEADS_DEV * 256), same),
                pl.BlockSpec(
                    (288, 1024),
                    lambda i, r: (r[0] + jnp.minimum(i, jnp.maximum(r[1] - 1, 0)), 0),
                ),
                pl.BlockSpec((512, 512), same),
                pl.BlockSpec((512, 512), same),
            ],
            out_specs=pl.BlockSpec((GROUP, 640), same),
            scratch_shapes=[
                pltpu.VMEM((GROUP, HEADS_DEV * 256), bf16),
                pltpu.VMEM((GROUP, HEADS_DEV * VDIM), bf16),
                pltpu.VMEM(state_shape, f32),
                pltpu.VMEM(state_shape, f32),
                pltpu.VMEM(state_shape, f32),
            ],
        ),
        compiler_params=pltpu.CompilerParams(dimension_semantics=("arbitrary",)),
        cost_estimate=pl.CostEstimate(
            flops=int(steps * 1.4e9), bytes_accessed=10000000, transcendentals=0
        ),
    )(plan, q, latents, w_key, w_value)


def on_device(
    q_latent,
    kv_latent,
    rope_key,
    gain_query,
    gain_latent,
    w_query,
    w_key,
    w_value,
    w_out,
    tokens_b,
    gain_norm,
    routes,
    route_weights,
    shared_gate,
    shared_up,
    shared_down,
    expert_gate,
    expert_up,
    expert_down,
):
    rank = lax.axis_index(EP)
    tp_rank = lax.axis_index("tp")
    regroup = jnp.asarray(regroup_matrix(), bf16)
    regroup_back = jnp.asarray(regroup_matrix().T, bf16)
    expert_gate, expert_up, expert_down = expert_gate[0], expert_up[0], expert_down[0]
    shared_w = (shared_gate, shared_up, shared_down)
    routed_w = (expert_gate, expert_up, expert_down)
    wire_shape = (N_EP * WIRE, CHUNK)

    def to_places(wire):
        got = lax.all_to_all(wire.reshape(N_EP, WIRE, CHUNK), EP, 0, 0, tiled=True)
        return got.reshape(wire_shape)

    def jump(x):
        return lax.ppermute(x, "tp", ring(2))

    def add(a, b):
        return (a.astype(f32) + b.astype(f32)).astype(bf16)

    before = (tp_rank - jnp.arange(N_TP, dtype=i32)) % N_TP
    positions = rank * GROUP + before[:, None] * ROWS + jnp.arange(ROWS, dtype=i32)[None, :]
    cos_tab, sin_tab = rope_angles(positions.reshape(GROUP), ROPE)

    s_lo, s_hi, wire = kernel_call(
        dispatch_body, (whole((64, WIDTH)), whole((64, WIDTH)), whole(wire_shape)), flops=2e9
    )(tokens_b, gain_norm.reshape(1, WIDTH), routes.T)
    sm_lo, sp_hi = up(s_lo), down(s_hi)
    sm_hi, sp_lo = up(s_hi), down(s_lo)
    arrived = to_places(wire)

    rope_in = after(rope_key, wire)
    rot_key = rotate_pairs(rope_in.astype(f32), cos_tab[:ROWS], sin_tab[:ROWS]).astype(bf16)
    rot_pair = jnp.concatenate([rot_key[:64], rot_key[64:]], axis=1)
    rot_rows = rot_pair.reshape(8, 8, 128).transpose(1, 0, 2).reshape(8, 1024)
    q_own, kv_own = kernel_call(prep_body, (whole((ROWS, 1024)), whole((72, 1024))))(
        q_latent, kv_latent, rot_rows, gain_query.reshape(1, -1), gain_latent.reshape(1, -1)
    )
    kv1, kv3, kv2 = up(kv_own), down(kv_own), jump(kv_own)
    latents = kernel_call(repack_body, whole((288, 1024)))(kv_own, kv1, kv2, kv3)
    latents_all = lax.all_gather(latents, EP, axis=0, tiled=True)
    q_tied = after(q_own, latents)
    q1, q3, q2 = up(q_tied), down(q_tied), jump(q_tied)
    routes_far = jump(after(routes, latents))
    weights_far = jump(after(route_weights, latents))

    x_lo, x_hi = kernel_call(unwire_body, (whole((HALF, WIDTH)),) * 2, flops=2e9)(
        after(arrived, latents), regroup
    )
    s2_lo, s2_hi = up(sm_lo), down(sp_hi)
    m_lo, p_hi = up(x_lo), down(x_hi)
    m_hi, p_lo = up(x_hi), down(x_lo)

    wire_far = kernel_call(dispatch_far_body, whole(wire_shape), flops=2e9)(
        after(s2_lo, x_lo), s2_hi, routes_far.T
    )
    arrived_far = to_places(wire_far)

    query_in = jnp.concatenate([after(q_own, wire_far), q1, q2, q3], axis=0)
    query_full = jnp.dot(query_in, w_query, preferred_element_type=f32)
    query_full = query_full.reshape(GROUP, HEADS_DEV, NOPE + ROPE)
    query_rot = rotate_pairs(
        query_full[:, :, NOPE:], cos_tab[:, None, :], sin_tab[:, None, :]
    ).astype(bf16)
    query_nope = query_full[:, :, :NOPE].astype(bf16)
    queries = jnp.concatenate([query_nope, query_rot, query_rot], axis=-1).reshape(GROUP, -1)
    pair_queries = lax.ppermute(queries, EP, [(N_EP - 1 - r, r) for r in range(N_EP // 2)])

    os_lo, os_hi = ffn((after(s_lo, queries), s_hi), *shared_w)
    own_lo, own_hi = ffn((after(x_lo, os_lo), x_hi), *routed_w)
    ms_lo, ms_hi, ps_lo, ps_hi = ffn((after(sm_lo, own_lo), sm_hi, sp_lo, sp_hi), *shared_w)
    ts_lo, ts_hi = ffn((after(s2_lo, ms_lo), s2_hi), *shared_w)
    mr_lo, mr_hi, pr_lo, pr_hi = ffn((after(m_lo, ts_lo), m_hi, p_lo, p_hi), *routed_w)
    fm_lo, fm_hi = up(pr_lo), up(pr_hi)
    fp_lo, fp_hi = down(mr_lo), down(mr_hi)
    f_lo, f_hi = kernel_call(unwire_body, (whole((HALF, WIDTH)),) * 2, flops=2e9)(
        after(arrived_far, mr_lo), regroup
    )
    fr_lo, fr_hi = ffn((f_lo, f_hi), *routed_w)
    back_far = kernel_call(rewire_body, whole(wire_shape), flops=2e9)(fr_lo, fr_hi, regroup_back)
    returned_far = to_places(back_far)

    heavy = (rank >= N_EP // 2).astype(i32)
    zero = jnp.zeros((), i32)
    pair_plan = jnp.stack([zero, jnp.maximum(N_EP // 2 - 1 - rank, 0), zero - 1, tp_rank])
    first = heavy * (rank - N_EP // 2)
    own_plan = jnp.stack([first, rank - first + 1, rank, tp_rank])
    pair_state = attend(15, pair_plan, after(pair_queries, back_far), latents_all, w_key, w_value)
    other_state = lax.ppermute(pair_state, EP, [(r, N_EP - 1 - r) for r in range(N_EP // 2)])
    own_state = attend(17, own_plan, after(queries, pair_state), latents_all, w_key, w_value)

    back = kernel_call(rewire_body, whole(wire_shape), flops=2e9)(
        after(own_lo, own_state), own_hi, fm_lo, fm_hi, fp_lo, fp_hi, regroup_back
    )
    returned = to_places(back)
    v_lo, v_hi = kernel_call(
        functools.partial(combine_body, 2), (whole((64, WIDTH)),) * 2, flops=3e9
    )(after(returned_far, back), routes_far, weights_far, ts_lo, ts_hi)
    svia_lo, svia_hi = up(v_lo), down(v_hi)
    sfm_hi, sfp_lo = up(after(ps_hi, mr_lo)), down(after(ms_lo, mr_lo))

    parts = kernel_call(out_body, (whole((64, WIDTH)),) * 8, flops=2e9, in_specs=OUT_SPECS)(
        heavy.reshape(1), after(own_state, v_lo), other_state, w_out
    )
    o_lo, o_hi, mo_lo, mo_hi, fo_lo, fo_hi, po_lo, po_hi = parts
    ovia_lo, ovia_hi = up(fo_lo), down(fo_hi)
    ofm_hi, ofp_lo = up(po_hi), down(mo_lo)
    sfm_lo = up(add(ps_lo, after(svia_lo, o_lo)))
    sfp_hi = down(add(ms_hi, after(svia_hi, o_lo)))
    ovia_lo, ovia_hi = after(ovia_lo, svia_lo), after(ovia_hi, svia_hi)
    ofm_lo, ofp_hi = up(add(po_lo, ovia_lo)), down(add(mo_hi, ovia_hi))

    expert_mix = kernel_call(combine_whole_body, whole((ROWS, WIDTH)), flops=3e9)(
        after(returned, o_lo),
        routes,
        route_weights,
        os_lo,
        os_hi,
        sfm_lo,
        sfm_hi,
        sfp_lo,
        sfp_hi,
    )
    mixer_out = kernel_call(sum_body, whole((ROWS, WIDTH)))(
        after(o_lo, expert_mix), o_hi, ofm_lo, ofm_hi, ofp_lo, ofp_hi
    )
    return (mixer_out, expert_mix)


def solution(mesh):
    finer = Mesh(mesh.devices.reshape(4, 4, 2, mesh.shape["tp"]), ("ep_0", "ep_1", "ep_2", "tp"))
    placed = (
        P(EP_TP, None),
        P(EP_TP, None),
        P(EP_TP, None),
        P(),
        P(),
        P(None, "tp"),
        P(None, "tp"),
        P(None, "tp"),
        P("tp", None),
        P(EP_TP, None),
        P(),
        P(EP_TP, None),
        P(EP_TP, None),
        P(None, "tp"),
        P(None, "tp"),
        P("tp", None),
        P(EP, None, "tp"),
        P(EP, None, "tp"),
        P(EP, "tp", None),
    )
    return jax.shard_map(
        on_device,
        mesh=finer,
        in_specs=placed,
        out_specs=(P(EP_TP, None), P(EP_TP, None)),
        check_vma=False,
    )
```

```python
import functools

import jax
import jax.numpy as jnp
import numpy as np
from jax import lax
from jax.experimental import pallas as pl
from jax.experimental.pallas import tpu as pltpu
from jax.sharding import Mesh
from jax.sharding import PartitionSpec as P

NOPE = 128
ROPE = 64
VDIM = 128
HEADS_DEV = 4
EP = ("ep_0", "ep_1", "ep_2")
EP_TP = ("ep_0", "ep_1", "ep_2", "tp")
N_EP = 32
N_TP = 4
ROWS = 128
GROUP = 512
WIDTH = 4096
CAP = 10
CHUNKS = 4
CHUNK = WIDTH // CHUNKS
WIRE = CAP * CHUNKS
SLOTS = N_EP * CAP
HALF = SLOTS // 2
SCALE = (NOPE + ROPE) ** (-0.5) * 1.4426950408889634

epsilon = 1e-06
rope_theta = 10000.0
bf16 = jnp.bfloat16
f32 = jnp.float32
i32 = jnp.int32


def whole(shape, dtype=bf16):
    return jax.ShapeDtypeStruct(shape, dtype)


def kernel_call(body, out_shape, flops=1000000, **kw):
    return pl.pallas_call(
        body,
        out_shape=out_shape,
        cost_estimate=pl.CostEstimate(flops=int(flops), bytes_accessed=1000000, transcendentals=0),
        **kw,
    )


def ring(steps):
    return [(i, (i + steps) % N_TP) for i in range(N_TP)]


def up(x):
    return lax.ppermute(x, "tp", ring(1))


def down(x):
    return lax.ppermute(x, "tp", ring(N_TP - 1))


def after(x, *deps):
    return lax.optimization_barrier((x, deps))[0]


def rope_angles(positions, rope_width):
    frequency = rope_theta ** (-jnp.arange(0, rope_width, 2, dtype=f32) / rope_width)
    angles = positions.astype(f32)[:, None] * frequency[None, :]
    return (jnp.cos(angles), jnp.sin(angles))


def rotate_pairs(values, cos_tab, sin_tab):
    half_width = values.shape[-1] // 2
    a = values[..., :half_width]
    b = values[..., half_width:]
    return jnp.concatenate([a * cos_tab - b * sin_tab, b * cos_tab + a * sin_tab], axis=-1)


def regroup_matrix():
    out = np.zeros((8 * WIRE, 8 * WIRE), np.float32)
    for c in range(CHUNKS):
        for s in range(8):
            for k in range(CAP):
                out[c * 8 * CAP + s * CAP + k, s * WIRE + c * CAP + k] = 1
    return out


def place(normed, routes_ref):
    r0 = routes_ref[0:1, :]
    r1 = routes_ref[1:2, :]
    expert = lax.broadcasted_iota(i32, (N_EP, ROWS), 0)
    hot0 = jnp.where(expert == r0, 1.0, 0.0)
    hot1 = jnp.where(expert == r1, 1.0, 0.0)
    before = lax.broadcasted_iota(i32, (ROWS, ROWS), 0) < lax.broadcasted_iota(i32, (ROWS, ROWS), 1)
    before = jnp.where(before, 1.0, 0.0).astype(bf16)
    seen0 = jnp.dot(hot0.astype(bf16), before, preferred_element_type=f32)
    seen1 = jnp.dot(hot1.astype(bf16), before, preferred_element_type=f32)
    seen1 = seen1 + jnp.sum(hot0, axis=1, keepdims=True)
    slot0 = jnp.sum(seen0 * hot0, axis=0, keepdims=True).astype(i32) + r0 * WIRE
    slot1 = jnp.sum(seen1 * hot1, axis=0, keepdims=True).astype(i32) + r1 * WIRE
    row = lax.broadcasted_iota(i32, (N_EP * WIRE, ROWS), 0)
    picks = jnp.concatenate(
        [
            jnp.where((row == slot0 + c * CAP) | (row == slot1 + c * CAP), 1.0, 0.0).astype(bf16)
            for c in range(CHUNKS)
        ],
        axis=1,
    )
    stacked = jnp.concatenate([normed[:, c * CHUNK : (c + 1) * CHUNK] for c in range(CHUNKS)], axis=0)
    return jnp.dot(picks, stacked, preferred_element_type=f32).astype(bf16)


def dispatch_body(tok_ref, gain_ref, routes_ref, lo_ref, hi_ref, wire_ref):
    x = tok_ref[...].astype(f32)
    mean = jnp.mean(x * x, axis=-1, keepdims=True)
    normed = ((x * lax.rsqrt(mean + epsilon)) * gain_ref[...]).astype(bf16)
    lo_ref[...] = normed[:64]
    hi_ref[...] = normed[64:]
    wire_ref[...] = place(normed, routes_ref)


def dispatch_far_body(lo_ref, hi_ref, routes_ref, wire_ref):
    wire_ref[...] = place(jnp.concatenate([lo_ref[...], hi_ref[...]], axis=0), routes_ref)


def unwire_body(wire_ref, mat_ref, lo_ref, hi_ref):
    mat = mat_ref[...]
    for g in range(4):
        got = jnp.dot(mat, wire_ref[g * 8 * WIRE : (g + 1) * 8 * WIRE, :], preferred_element_type=f32)
        got = got.astype(bf16)
        out_ref = lo_ref if g < 2 else hi_ref
        base = (g % 2) * 8 * CAP
        for c in range(CHUNKS):
            out_ref[base : base + 8 * CAP, c * CHUNK : (c + 1) * CHUNK] = got[c * 8 * CAP : (c + 1) * 8 * CAP, :]


def rewire_body(*refs):
    parts, mat, wire_ref = refs[:-2], refs[-2][...], refs[-1]
    for g in range(4):
        base = (g % 2) * 8 * CAP
        pieces = []
        for c in range(CHUNKS):
            sl = (slice(base, base + 8 * CAP), slice(c * CHUNK, (c + 1) * CHUNK))
            terms = [part[sl] for part in parts[g // 2 :: 2]]
            if len(terms) == 1:
                pieces.append(terms[0])
            else:
                total = terms[0].astype(f32)
                for term in terms[1:]:
                    total = total + term.astype(f32)
                pieces.append(total.astype(bf16))
        rows = jnp.concatenate(pieces, axis=0)
        got = jnp.dot(mat, rows, preferred_element_type=f32)
        wire_ref[g * 8 * WIRE : (g + 1) * 8 * WIRE, :] = got.astype(bf16)


def ffn_body(count, block, *refs):
    xs, (gate, upw, downw), outs = refs[:count], refs[count : count + 3], refs[count + 3 : 2 * count + 3]
    x_all, y_all = refs[2 * count + 3 :]
    rows = xs[0].shape[0]
    for k, x_ref in enumerate(xs):
        x_all[k * rows : (k + 1) * rows, :] = x_ref[...]

    @pl.loop(0, count * rows // block)
    def _(i):
        here = pl.ds(pl.multiple_of(i * block, block), block)
        x = x_all[here, :]
        g = jnp.dot(x, gate[...], preferred_element_type=f32)
        u = jnp.dot(x, upw[...], preferred_element_type=f32)
        hidden = ((g / (1.0 + jnp.exp(-g))) * u).astype(bf16)
        y_all[here, :] = jnp.dot(hidden, downw[...], preferred_element_type=f32).astype(bf16)

    for k, out_ref in enumerate(outs):
        out_ref[...] = y_all[k * rows : (k + 1) * rows, :]


def ffn(xs, gate, upw, downw, block):
    rows = sum(x.shape[0] for x in xs)
    call = kernel_call(
        functools.partial(ffn_body, len(xs), block),
        tuple(whole(x.shape) for x in xs),
        flops=rows * WIDTH * 256 * 6,
        scratch_shapes=[pltpu.VMEM((rows, WIDTH), bf16)] * 2,
    )
    return call(*xs, gate, upw, downw)


def combine_body(count, *refs):
    ret_ref, routes_ref, rw_ref = refs[:3]
    shared, (lo_ref, hi_ref) = refs[3 : 3 + count], refs[3 + count :]
    r0 = routes_ref[:, 0:1]
    r1 = routes_ref[:, 1:2]
    expert = lax.broadcasted_iota(i32, (ROWS, N_EP), 1)
    hot0 = jnp.where(expert == r0, 1.0, 0.0)
    hot1 = jnp.where(expert == r1, 1.0, 0.0)
    before = lax.broadcasted_iota(i32, (ROWS, ROWS), 1) < lax.broadcasted_iota(i32, (ROWS, ROWS), 0)
    before = jnp.where(before, 1.0, 0.0).astype(bf16)
    seen0 = jnp.dot(before, hot0.astype(bf16), preferred_element_type=f32)
    seen1 = jnp.dot(before, hot1.astype(bf16), preferred_element_type=f32)
    seen1 = seen1 + jnp.sum(hot0, axis=0, keepdims=True)
    slot0 = jnp.sum(seen0 * hot0, axis=1, keepdims=True).astype(i32) + r0 * WIRE
    slot1 = jnp.sum(seen1 * hot1, axis=1, keepdims=True).astype(i32) + r1 * WIRE
    col = lax.broadcasted_iota(i32, (ROWS, N_EP * WIRE), 1)
    w0 = rw_ref[:, 0:1]
    w1 = rw_ref[:, 1:2]
    ret = ret_ref[...]
    for c in range(CHUNKS):
        picks = jnp.concatenate(
            [
                jnp.where(col == slot0 + c * CAP, 1.0, 0.0).astype(bf16),
                jnp.where(col == slot1 + c * CAP, 1.0, 0.0).astype(bf16),
            ],
            axis=0,
        )
        got = jnp.dot(picks, ret, preferred_element_type=f32)
        routed = w0 * got[:ROWS] + w1 * got[ROWS:]
        cols = slice(c * CHUNK, (c + 1) * CHUNK)
        for h, out_ref in ((0, lo_ref), (1, hi_ref)):
            total = routed[h * 64 : h * 64 + 64]
            for part in shared[h::2]:
                total = total + part[:, cols].astype(f32)
            if out_ref.shape[0] == ROWS:
                lo_ref[h * 64 : h * 64 + 64, cols] = total.astype(bf16)
            else:
                out_ref[:, cols] = total.astype(bf16)


def combine_whole_body(*refs):
    combine_body(6, *refs, refs[-1])


def sum_body(*refs):
    out_ref = refs[-1]
    for h in range(2):
        total = refs[h][...].astype(f32) + refs[2 + h][...].astype(f32) + refs[4 + h][...].astype(f32)
        out_ref[h * 64 : h * 64 + 64, :] = total.astype(bf16)


OUT_SPECS = [pl.BlockSpec(memory_space=pltpu.SMEM)] + [pl.BlockSpec(memory_space=pltpu.VMEM)] * 3


def out_body(heavy_ref, own_ref, other_ref, w_ref, *outs):
    heads = []
    for h in range(HEADS_DEV):
        cols = slice(h * 128, (h + 1) * 128)
        m_own, l_own = own_ref[:, 512 + h : 513 + h], own_ref[:, 516 + h : 517 + h]
        m_other, l_other = other_ref[:, 512 + h : 513 + h], other_ref[:, 516 + h : 517 + h]
        m_other = jnp.where(heavy_ref[0] > 0, m_other, -jnp.inf)
        top = jnp.maximum(m_own, m_other)
        f_own = jnp.exp2((m_own - top) * SCALE)
        f_other = jnp.exp2((m_other - top) * SCALE)
        total = l_own * f_own + l_other * f_other
        acc = own_ref[:, cols] * f_own + other_ref[:, cols] * f_other
        heads.append((acc / total).astype(bf16))
    got = jnp.dot(jnp.concatenate(heads, axis=1), w_ref[...], preferred_element_type=f32).astype(bf16)
    for k, out_ref in enumerate(outs):
        out_ref[...] = got[k * 64 : (k + 1) * 64]


def prep_body(q_ref, kv_ref, rot_ref, gq_ref, gkv_ref, *outs):
    def norm(ref, gain):
        x = ref[...].astype(f32)
        mean = jnp.mean(x * x, axis=-1, keepdims=True)
        return ((x * lax.rsqrt(mean + epsilon)) * gain[...]).astype(bf16)

    q_out, kv_out = outs
    q_out[...] = norm(q_ref, gq_ref)
    kv = norm(kv_ref, gkv_ref)
    kv_out[0:64, 0:512] = kv[:64]
    kv_out[0:64, 512:1024] = kv[64:]
    kv_out[64:72, :] = rot_ref[...]


def repack_body(*refs):
    out_ref = refs[-1]
    for j in range(N_TP):
        out_ref[j * 64 : (j + 1) * 64, :] = refs[j][0:64, :]
        rot = refs[j][64:72, :].astype(f32)
        for half in range(2):
            piece = [rot[:, g * 128 : (g + 1) * 128] for g in range(4 * half, 4 * half + 4)]
            g = 2 * j + half
            out_ref[256:288, g * 128 : (g + 1) * 128] = jnp.concatenate(piece, axis=0).astype(bf16)


def attend_body(diagonal_too, plan_ref, q_ref, lat_ref, wk_ref, wv_ref, out_ref, kcat, val, m_ref, l_ref, acc_ref):
    step = pl.program_id(0)
    block = step + plan_ref[0]

    @pl.when(step == 0)
    def _():
        m_ref[...] = jnp.full(m_ref.shape, -jnp.inf, f32)
        l_ref[...] = jnp.zeros(l_ref.shape, f32)
        acc_ref[...] = jnp.zeros(acc_ref.shape, f32)

    def work(diagonal):
        low = lax.broadcasted_iota(i32, (256, 128), 1) < ROPE
        zero = jnp.zeros((256, 128), bf16)
        pair = jnp.concatenate([lat_ref[256:288, g * 128 : (g + 1) * 128] for g in range(8)], axis=0)
        for half in range(2):
            kv = lat_ref[0:256, half * 512 : half * 512 + 512]
            rows = slice(half * 256, half * 256 + 256)
            keys = jnp.dot(kv, wk_ref[...], preferred_element_type=f32).astype(bf16)
            val[rows, :] = jnp.dot(kv, wv_ref[...], preferred_element_type=f32).astype(bf16)
            rot = jnp.where(low, pair, zero) if half == 0 else jnp.where(low, zero, pair)
            for h in range(HEADS_DEV):
                kcat[rows, h * 256 : h * 256 + 128] = keys[:, h * 128 : (h + 1) * 128]
                kcat[rows, h * 256 + 128 : (h + 1) * 256] = rot

        def score(h):
            return lax.dot_general(
                q_ref[:, h * 256 : (h + 1) * 256],
                kcat[:, h * 256 : (h + 1) * 256],
                (((1,), (1,)), ((), ())),
                preferred_element_type=f32,
            )

        ahead = score(0)
        for h in range(HEADS_DEV):
            scores = ahead
            if h + 1 < HEADS_DEV:
                ahead = score(h + 1)
            if diagonal:
                row = lax.broadcasted_iota(i32, (GROUP, GROUP), 0)
                col = lax.broadcasted_iota(i32, (GROUP, GROUP), 1)
                row = ((plan_ref[3] - (row >> 7)) & 3) * 128 + (row & 127)
                piece = (plan_ref[3] - ((col & 255) >> 6)) & 3
                col = piece * 128 + (col >> 8) * 64 + (col & 63)
                scores = jnp.where(row >= col, scores, -jnp.inf)
            m_old = m_ref[h]
            m_new = jnp.maximum(m_old, jnp.max(scores, axis=-1, keepdims=True))
            factor = jnp.exp2((m_old - m_new) * SCALE)
            wide = jnp.concatenate([m_new] * 4, axis=1)
            terms = jnp.exp2((scores - wide) * SCALE)
            part = (terms[:, 0:128] + terms[:, 128:256]) + (terms[:, 256:384] + terms[:, 384:512])
            m_ref[h] = m_new
            l_ref[h] = l_ref[h] * factor + part
            update = jnp.dot(
                terms.astype(bf16), val[:, h * 128 : (h + 1) * 128], preferred_element_type=f32
            )
            acc_ref[h] = acc_ref[h] * factor + update

    @pl.when((step < plan_ref[1]) & (block != plan_ref[2]))
    def _():
        work(False)

    if diagonal_too:

        @pl.when((step < plan_ref[1]) & (block == plan_ref[2]))
        def _():
            work(True)

    @pl.when(step == pl.num_programs(0) - 1)
    def _():
        lane = lax.broadcasted_iota(i32, (GROUP, 128), 1)
        stats = jnp.zeros((GROUP, 128), f32)
        for h in range(HEADS_DEV):
            out_ref[:, h * 128 : (h + 1) * 128] = acc_ref[h]
            stats = jnp.where(lane == h, m_ref[h], stats)
            stats = jnp.where(lane == 4 + h, jnp.sum(l_ref[h], axis=-1, keepdims=True), stats)
        out_ref[:, 512:640] = stats


def attend(diagonal_too, steps, plan, q, latents, w_key, w_value):
    state_shape = (HEADS_DEV, GROUP, 128)
    same = lambda i, r: (0, 0)
    return pl.pallas_call(
        functools.partial(attend_body, diagonal_too),
        out_shape=whole((GROUP, 640), f32),
        grid_spec=pltpu.PrefetchScalarGridSpec(
            num_scalar_prefetch=1,
            grid=(steps,),
            in_specs=[
                pl.BlockSpec((GROUP, HEADS_DEV * 256), same),
                pl.BlockSpec(
                    (288, 1024),
                    lambda i, r: (r[0] + jnp.minimum(i, jnp.maximum(r[1] - 1, 0)), 0),
                ),
                pl.BlockSpec((512, 512), same),
                pl.BlockSpec((512, 512), same),
            ],
            out_specs=pl.BlockSpec((GROUP, 640), same),
            scratch_shapes=[
                pltpu.VMEM((GROUP, HEADS_DEV * 256), bf16),
                pltpu.VMEM((GROUP, HEADS_DEV * VDIM), bf16),
                pltpu.VMEM(state_shape, f32),
                pltpu.VMEM(state_shape, f32),
                pltpu.VMEM(state_shape, f32),
            ],
        ),
        compiler_params=pltpu.CompilerParams(dimension_semantics=("arbitrary",)),
        cost_estimate=pl.CostEstimate(
            flops=int(17 * 1.4e9), bytes_accessed=10000000, transcendentals=0
        ),
    )(plan, q, latents, w_key, w_value)


def on_device(
    q_latent,
    kv_latent,
    rope_key,
    gain_query,
    gain_latent,
    w_query,
    w_key,
    w_value,
    w_out,
    tokens_b,
    gain_norm,
    routes,
    route_weights,
    shared_gate,
    shared_up,
    shared_down,
    expert_gate,
    expert_up,
    expert_down,
):
    rank = lax.axis_index(EP)
    tp_rank = lax.axis_index("tp")
    regroup = jnp.asarray(regroup_matrix(), bf16)
    regroup_back = jnp.asarray(regroup_matrix().T, bf16)
    expert_gate, expert_up, expert_down = expert_gate[0], expert_up[0], expert_down[0]
    shared_w = (shared_gate, shared_up, shared_down)
    routed_w = (expert_gate, expert_up, expert_down)
    wire_shape = (N_EP * WIRE, CHUNK)

    def to_places(wire):
        got = lax.all_to_all(wire.reshape(N_EP, WIRE, CHUNK), EP, 0, 0, tiled=True)
        return got.reshape(wire_shape)

    def jump(x):
        return lax.ppermute(x, "tp", ring(2))

    def add(a, b):
        return (a.astype(f32) + b.astype(f32)).astype(bf16)

    before = (tp_rank - jnp.arange(N_TP, dtype=i32)) % N_TP
    positions = rank * GROUP + before[:, None] * ROWS + jnp.arange(ROWS, dtype=i32)[None, :]
    cos_tab, sin_tab = rope_angles(positions.reshape(GROUP), ROPE)

    s_lo, s_hi, wire = kernel_call(
        dispatch_body, (whole((64, WIDTH)), whole((64, WIDTH)), whole(wire_shape)), flops=2e9
    )(tokens_b, gain_norm.reshape(1, WIDTH), routes.T)
    arrived = to_places(wire)
    routes_far = jump(after(routes, wire))
    weights_far = jump(after(route_weights, wire))

    rope_in = after(rope_key, wire)
    rot_key = rotate_pairs(rope_in.astype(f32), cos_tab[:ROWS], sin_tab[:ROWS]).astype(bf16)
    rot_pair = jnp.concatenate([rot_key[:64], rot_key[64:]], axis=1)
    rot_rows = rot_pair.reshape(8, 8, 128).transpose(1, 0, 2).reshape(8, 1024)
    q_own, kv_own = kernel_call(prep_body, (whole((ROWS, 1024)), whole((72, 1024))))(
        q_latent, kv_latent, rot_rows, gain_query.reshape(1, -1), gain_latent.reshape(1, -1)
    )
    kv1, kv3, kv2 = up(kv_own), down(kv_own), jump(kv_own)
    s_lo, s_hi = lax.optimization_barrier(((s_lo, s_hi), kv_own))[0]
    sm_lo, sp_hi = up(s_lo), down(s_hi)
    latents = kernel_call(repack_body, whole((288, 1024)))(kv_own, kv1, kv2, kv3)
    latents_all = lax.all_gather(latents, EP, axis=0, tiled=True)
    q_tied = after(q_own, latents)
    q1, q3, q2 = up(q_tied), down(q_tied), jump(q_tied)

    x_lo, x_hi = kernel_call(unwire_body, (whole((HALF, WIDTH)),) * 2, flops=2e9)(
        after(arrived, latents), regroup
    )
    s2_lo, s2_hi = up(sm_lo), down(sp_hi)
    sm_hi, sp_lo = up(after(s_hi, latents)), down(after(s_lo, latents))
    m_lo, p_hi = up(x_lo), down(x_hi)
    m_hi, p_lo = up(x_hi), down(x_lo)

    wire_far = kernel_call(dispatch_far_body, whole(wire_shape), flops=2e9)(
        after(s2_lo, x_lo), s2_hi, routes_far.T
    )
    arrived_far = to_places(wire_far)

    query_in = jnp.concatenate([after(q_own, wire_far), q1, q2, q3], axis=0)
    query_full = jnp.dot(query_in, w_query, preferred_element_type=f32)
    query_full = query_full.reshape(GROUP, HEADS_DEV, NOPE + ROPE)
    query_rot = rotate_pairs(
        query_full[:, :, NOPE:], cos_tab[:, None, :], sin_tab[:, None, :]
    ).astype(bf16)
    query_nope = query_full[:, :, :NOPE].astype(bf16)
    queries = jnp.concatenate([query_nope, query_rot, query_rot], axis=-1).reshape(GROUP, -1)
    pair_queries = lax.ppermute(queries, EP, [(N_EP - 1 - r, r) for r in range(N_EP // 2)])

    os_lo, os_hi, ms_lo, ms_hi, ps_lo, ps_hi, ts_lo, ts_hi = ffn(
        (after(s_lo, queries), s_hi, sm_lo, sm_hi, sp_lo, sp_hi, s2_lo, s2_hi), *shared_w, 256
    )
    own_lo, own_hi = ffn((after(x_lo, os_lo), x_hi), *routed_w, 320)
    mr_lo, mr_hi, pr_lo, pr_hi = ffn((after(m_lo, own_lo), m_hi, p_lo, p_hi), *routed_w, 320)
    fm_lo, fm_hi = up(pr_lo), up(pr_hi)
    fp_lo, fp_hi = down(mr_lo), down(mr_hi)
    f_lo, f_hi = kernel_call(unwire_body, (whole((HALF, WIDTH)),) * 2, flops=2e9)(
        after(arrived_far, mr_lo), regroup
    )
    fr_lo, fr_hi = ffn((f_lo, f_hi), *routed_w, 320)
    back_far = kernel_call(rewire_body, whole(wire_shape), flops=2e9)(fr_lo, fr_hi, regroup_back)
    returned_far = to_places(back_far)

    heavy = (rank >= N_EP // 2).astype(i32)
    zero = jnp.zeros((), i32)
    pair_plan = jnp.stack([zero, jnp.maximum(N_EP // 2 - 1 - rank, 0), zero - 1, tp_rank])
    first = heavy * (rank - N_EP // 2)
    own_plan = jnp.stack([first, rank - first + 1, rank, tp_rank])
    pair_state = attend(
        False, 15, pair_plan, after(pair_queries, back_far), latents_all, w_key, w_value
    )
    other_state = lax.ppermute(pair_state, EP, [(r, N_EP - 1 - r) for r in range(N_EP // 2)])
    own_state = attend(True, 17, own_plan, after(queries, pair_state), latents_all, w_key, w_value)

    v_lo, v_hi = kernel_call(
        functools.partial(combine_body, 2), (whole((64, WIDTH)),) * 2, flops=3e9
    )(after(returned_far, own_state), routes_far, weights_far, ts_lo, ts_hi)
    svia_lo, svia_hi = up(v_lo), down(v_hi)
    sfm_hi, sfp_lo = up(after(ps_hi, mr_lo)), down(after(ms_lo, mr_lo))
    back = kernel_call(rewire_body, whole(wire_shape), flops=2e9)(
        after(own_lo, v_lo), own_hi, fm_lo, fm_hi, fp_lo, fp_hi, regroup_back
    )
    returned = to_places(back)
    sfm_lo = up(add(ps_lo, after(svia_lo, back)))
    sfp_hi = down(add(ms_hi, after(svia_hi, back)))
    parts = kernel_call(out_body, (whole((64, WIDTH)),) * 8, flops=2e9, in_specs=OUT_SPECS)(
        heavy.reshape(1), after(own_state, back), other_state, w_out
    )
    o_lo, o_hi, mo_lo, mo_hi, fo_lo, fo_hi, po_lo, po_hi = parts
    ovia_lo, ovia_hi = up(fo_lo), down(fo_hi)
    ofm_hi, ofp_lo = up(po_hi), down(mo_lo)
    ofm_lo = up(add(po_lo, after(ovia_lo, o_lo)))
    ofp_hi = down(add(mo_hi, after(ovia_hi, o_lo)))

    expert_mix = kernel_call(combine_whole_body, whole((ROWS, WIDTH)), flops=3e9)(
        returned,
        routes,
        route_weights,
        os_lo,
        os_hi,
        sfm_lo,
        sfm_hi,
        sfp_lo,
        sfp_hi,
    )
    mixer_out = kernel_call(sum_body, whole((ROWS, WIDTH)))(
        after(o_lo, expert_mix), o_hi, ofm_lo, ofm_hi, ofp_lo, ofp_hi
    )
    return (mixer_out, expert_mix)


def solution(mesh):
    finer = Mesh(mesh.devices.reshape(4, 4, 2, mesh.shape["tp"]), ("ep_0", "ep_1", "ep_2", "tp"))
    placed = (
        P(EP_TP, None),
        P(EP_TP, None),
        P(EP_TP, None),
        P(),
        P(),
        P(None, "tp"),
        P(None, "tp"),
        P(None, "tp"),
        P("tp", None),
        P(EP_TP, None),
        P(),
        P(EP_TP, None),
        P(EP_TP, None),
        P(None, "tp"),
        P(None, "tp"),
        P("tp", None),
        P(EP, None, "tp"),
        P(EP, None, "tp"),
        P(EP, "tp", None),
    )
    return jax.shard_map(
        on_device,
        mesh=finer,
        in_specs=placed,
        out_specs=(P(EP_TP, None), P(EP_TP, None)),
        check_vma=False,
    )
```
